32 devices in a mesh: kv: 8 (over z, x), tp: 4 (over y, core).
Axes of the slice: x: 2, y: 2, z: 4, core: 2. Of those that a mesh axis runs over, the one named last changes fastest.
Arguments:
- tokens: bfloat16 [32, 2048], P(None, 'kv'), may hold values from -6 to 6
- token_gain: float32 [2048], P('kv'), may hold values from 0.1 to 1.9
- w_query: bfloat16 [2048, 1536], P('kv', 'tp'), may hold values from -0.125 to 0.125
- w_down_kv: bfloat16 [2048, 512], P('kv'), may hold values from -0.125 to 0.125
- w_rope_key: bfloat16 [2048, 64], P('kv'), may hold values from -0.125 to 0.125
- latent_gain: float32 [512], replicated, may hold values from 0.1 to 1.9
- w_key_up: bfloat16 [8, 512, 128], P('tp'), may hold values from -0.25 to 0.25
- w_value_up: bfloat16 [8, 512, 128], P('tp'), may hold values from -0.25 to 0.25
- w_out: bfloat16 [1024, 2048], P('tp', 'kv'), may hold values from -0.1875 to 0.1875
- out_gain: float32 [2048], P('kv'), may hold values from 0.1 to 1.9
- cache_latent: bfloat16 [32, 4096, 512], P('tp', 'kv'), may hold values from -6 to 6
- cache_rope: bfloat16 [32, 4096, 64], P('tp', 'kv'), may hold values from -6 to 6
- lengths: int32 [32], replicated, may hold values from 1 to 4095, as said below
Outputs:
- mixed: bfloat16 [32, 2048], P(None, 'kv')
The draws below stay inside these ranges and needn't reach their ends.
Inputs may be any that keep to these rules, and one draw needn't show every extreme that they name: `lengths`: each of the 32 sequences has 1 to 4095 cached positions; some sequence has exactly 4095 and some exactly 1.
All inputs are finite; a program needn't handle non-finite values.
Results may differ from the reference program's by a relative error of at most 0.015.
Values may be sent and summed in bfloat16 or wider, within the bound.
A program may use at most 64 MiB of HBM per device.

```python
import jax
import jax.numpy as jnp
from jax import lax

D = 2048
HEADS = 8
LATENT = 512
NOPE = 128
ROPE = 64
VDIM = 128
BATCH = 32
CACHE_LEN = 4096


def draw_lengths(key, part):
    first_key, second_key = jax.random.split(jax.random.fold_in(key, 11))
    first_draw = jax.random.randint(first_key, (BATCH,), 1, CACHE_LEN)
    second_draw = jax.random.randint(second_key, (BATCH,), 1, CACHE_LEN)
    joined = jnp.minimum(first_draw, second_draw)
    joined = joined.at[0].set(CACHE_LEN - 1).at[BATCH - 1].set(1)
    return joined.astype(jnp.int32)


def block_scale(stream_key, extent, shards, least, high):
    def one(axis_at, shards_of):
        heights = jax.random.uniform(jax.random.fold_in(jax.random.fold_in(stream_key, 6), axis_at), (shards_of,), jnp.float32, least / len(shards), high / len(shards))
        return jnp.repeat(jnp.exp(heights), extent[axis_at] // shards_of).reshape((-1,) + (1,) * (len(extent) - axis_at - 1))

    gain = one(*shards[0])
    for cut in shards[1:]:
        gain = gain * one(*cut)
    return gain


def centred(stream_key, shape, spread, limit, pieces=(), kind=jnp.bfloat16):
    values = jax.random.normal(stream_key, shape, jnp.float32) * spread
    if len(pieces) > 0:
        values = block_scale(stream_key, shape, pieces, -0.22, 0.18) * values
    return jnp.clip(values, min=-limit, max=limit).astype(kind)


def setup_inputs(seed: int = 0) -> dict:
    keys = jax.random.split(jax.random.key(seed), 14)
    return {
        "tokens": centred(keys[0], (BATCH, D), 1.0, 6.0, ((1, 8),)),
        "token_gain": jnp.clip(1.0 + 0.18 * jax.random.normal(keys[1], (D,), jnp.float32), 0.1, 1.9),
        "w_query": centred(keys[2], (D, HEADS * (NOPE + ROPE)), D ** -0.5, 0.125, ((0, 8), (1, 4))),
        "w_down_kv": centred(keys[3], (D, LATENT), D ** -0.5, 0.125, ((0, 8),)),
        "w_rope_key": centred(keys[4], (D, ROPE), D ** -0.5, 0.125, ((0, 8),)),
        "latent_gain": jnp.clip(1.0 + 0.18 * jax.random.normal(keys[5], (LATENT,), jnp.float32), 0.1, 1.9),
        "w_key_up": centred(keys[6], (HEADS, LATENT, NOPE), LATENT ** -0.5, 0.25, ((0, 4),)),
        "w_value_up": centred(keys[7], (HEADS, LATENT, VDIM), LATENT ** -0.5, 0.25, ((0, 4),)),
        "w_out": centred(keys[8], (HEADS * VDIM, D), (HEADS * VDIM) ** -0.5, 0.1875, ((0, 4), (1, 8))),
        "out_gain": jnp.clip(1.0 + 0.18 * jax.random.normal(keys[9], (D,), jnp.float32), 0.1, 1.9),
        "cache_latent": centred(keys[10], (BATCH, CACHE_LEN, LATENT), 1.0, 6.0, ((0, 4), (1, 8))),
        "cache_rope": centred(keys[11], (BATCH, CACHE_LEN, ROPE), 1.0, 6.0, ((0, 4), (1, 8))),
        "lengths": draw_lengths(jax.random.fold_in(keys[13], 71), 0),
    }


EPSILON = 1e-06
NEGATIVE = -1e+30

def rotate_half(values, cosine, sine_table):
    half_width = values.shape[-1] // 2
    lower_half = values[..., :half_width]
    upper_half = values[..., half_width:]
    return jnp.concatenate([lower_half * cosine - upper_half * sine_table, upper_half * cosine + lower_half * sine_table], axis=-1)

def angle_tables(lengths, rope_width):
    inverse_freq = 1.0 / 10000.0 ** (jnp.arange(0, rope_width, 2, dtype=jnp.float32) / rope_width)
    angles = lengths.astype(jnp.float32)[:, None] * inverse_freq[None, :]
    return (jnp.cos(angles), jnp.sin(angles))

def attend_one(packed):
    query_lat, query_rot, new_latent, new_key, length, cached_lat, cached_rot = packed
    factor = (NOPE + ROPE) ** (-0.5)
    scores = (jnp.dot(query_lat, cached_lat.T, preferred_element_type=jnp.float32) + jnp.dot(query_rot, cached_rot.T, preferred_element_type=jnp.float32)) * factor
    new_score = (jnp.dot(query_lat, new_latent, preferred_element_type=jnp.float32) + jnp.dot(query_rot, new_key, preferred_element_type=jnp.float32)) * factor
    visible = jnp.arange(CACHE_LEN) < length
    top_score = jnp.maximum(lax.optimization_barrier(jnp.max(jnp.where(visible[None, :], scores, NEGATIVE), axis=1)), new_score)
    weights = jnp.where(visible[None, :], jnp.exp(scores - top_score[:, None]), jnp.float32(0.0))
    new_weight = jnp.exp(new_score - top_score)
    weight_sum = lax.optimization_barrier(jnp.sum(weights, axis=1)) + new_weight
    rounded_new = lax.optimization_barrier(new_weight.astype(jnp.bfloat16)).astype(jnp.float32)
    weighted = jnp.dot(weights.astype(jnp.bfloat16), cached_lat, preferred_element_type=jnp.float32) + rounded_new[:, None] * new_latent.astype(jnp.float32)[None, :]
    return (weighted / weight_sum[:, None]).astype(jnp.bfloat16)

def reference(tokens, token_gain, w_query, w_down_kv, w_rope_key, latent_gain, w_key_up, w_value_up, w_out, out_gain, cache_latent, cache_rope, lengths):
    token_values = tokens.astype(jnp.float32)
    scaled = (token_values * token_gain).astype(jnp.bfloat16)
    query_heads = jnp.dot(scaled, w_query, preferred_element_type=jnp.float32).astype(jnp.bfloat16).reshape(BATCH, HEADS, NOPE + ROPE)
    latent_raw = jnp.dot(scaled, w_down_kv, preferred_element_type=jnp.float32)
    rope_raw = jnp.dot(scaled, w_rope_key, preferred_element_type=jnp.float32)
    latent = (latent_raw * lax.rsqrt(lax.optimization_barrier(jnp.mean(latent_raw * latent_raw, axis=1, keepdims=True)) + EPSILON) * latent_gain).astype(jnp.bfloat16)
    cosine, sine_table = angle_tables(lengths, ROPE)
    new_rope = rotate_half(rope_raw, cosine, sine_table).astype(jnp.bfloat16)
    query_nope = query_heads[..., :NOPE]
    query_rope = rotate_half(query_heads[..., NOPE:].astype(jnp.float32), cosine[:, None, :], sine_table[:, None, :]).astype(jnp.bfloat16)
    query_latent = jnp.einsum('bhn,hcn->bhc', query_nope.astype(jnp.float32), w_key_up.astype(jnp.float32)).astype(jnp.bfloat16)
    head_latent = lax.map(attend_one, (query_latent, query_rope, latent, new_rope, lengths, cache_latent, cache_rope))
    head_out = jnp.einsum('bhc,hcv->bhv', head_latent.astype(jnp.float32), w_value_up.astype(jnp.float32)).astype(jnp.bfloat16).reshape(BATCH, HEADS * VDIM)
    mixed_sum = jnp.dot(head_out, w_out, preferred_element_type=jnp.float32)
    out_inverse = lax.rsqrt(lax.optimization_barrier(jnp.mean(mixed_sum * mixed_sum, axis=1)) + EPSILON)[:, None]
    return (mixed_sum * out_inverse * out_gain).astype(jnp.bfloat16)
```

```python
import functools

import jax
import jax.numpy as jnp
from jax import lax
from jax.experimental import pallas as pl
from jax.experimental.pallas import tpu as pltpu
from jax.sharding import PartitionSpec as P

EPSILON = 1e-06
NEGATIVE = -1e30
LANES = 128
MESH = pl.DeviceIdType.MESH
F32 = jnp.float32
BF16 = jnp.bfloat16


def rounded(values):
    return values.astype(BF16).astype(F32)


def rotated(values, cosine, signed_sine, half):
    lane = lax.broadcasted_iota(jnp.int32, values.shape, 1)
    swapped = jnp.where(
        lane < half, pltpu.roll(values, LANES - half, 1), pltpu.roll(values, half, 1)
    )
    return values * cosine + swapped * signed_sine


def dot_t(a, b):
    return lax.dot_general(a, b, (((1,), (1,)), ((), ())), preferred_element_type=F32)


def kernel(
    kv,
    tp,
    lengths,
    tok_h,
    tgain_h,
    wq_h,
    wd_h,
    wr_h,
    cos_h,
    sin_h,
    wku_h,
    cl_h,
    cr_h,
    lgain_h,
    wvu_h,
    wo_h,
    ogain_h,
    out,
    tok,
    tgain,
    wq,
    wd,
    wr,
    cos,
    sin,
    wku,
    cl,
    cr,
    lgain,
    wvu,
    wo,
    ogain,
    scaled_s,
    q_send,
    q_recv,
    lat_send,
    lat_recv,
    row_send,
    row_recv,
    ql_send,
    ql_recv,
    q32,
    stage,
    part_send,
    part_recv,
    hl_send,
    hl_recv,
    mix_send,
    mix_recv,
    sq_send,
    sq_recv,
    in_sem,
    q_ss,
    q_rs,
    lat_ss,
    lat_rs,
    row_ss,
    row_rs,
    ql_ss,
    ql_rs,
    part_ss,
    part_rs,
    hl_ss,
    hl_rs,
    mix_ss,
    mix_rs,
    sq_ss,
    sq_rs,
):
    k = lax.axis_index("kv")
    t = lax.axis_index("tp")
    batch, width = tok.shape
    lh, latent, nope_w = wku.shape
    rope_w = wr.shape[1]
    head_w = nope_w + rope_w
    half = rope_w // 2
    factor = head_w ** (-0.5)
    seqs, pos = cl.shape[0], cl.shape[1]
    heads = lh * tp
    full = latent + LANES
    per_row = kv // tp
    dup = per_row // lh
    lat_dup = kv // seqs
    rows = heads * seqs // kv
    parts = seqs // rows
    model_w = width * kv
    chunk = q_send.shape[2]

    loads = [
        pltpu.make_async_copy(a, b, in_sem.at[i])
        for i, (a, b) in enumerate(
            [
                (tok_h, tok),
                (tgain_h, tgain),
                (wq_h, wq),
                (wd_h, wd),
                (wr_h, wr),
                (cos_h, cos),
                (sin_h, sin),
                (wku_h, wku),
                (lgain_h, lgain),
                (cl_h, cl),
                (cr_h, cr),
                (wvu_h, wvu),
                (wo_h, wo),
                (ogain_h, ogain),
            ]
        )
    ]
    for load in loads:
        load.start()

    barrier = pltpu.get_barrier_semaphore()
    me = k * tp + t

    def greet(i, carry):
        @pl.when(i != me)
        def _():
            pl.semaphore_signal(
                barrier, inc=1, device_id=(i // tp, i % tp), device_id_type=MESH
            )

        return carry

    lax.fori_loop(0, kv * tp, greet, 0)

    def remote(src, dst, send, recv, kk, tt):
        return pltpu.make_async_remote_copy(
            src_ref=src,
            dst_ref=dst,
            send_sem=send,
            recv_sem=recv,
            device_id=(kk, tt),
            device_id_type=MESH,
        )

    def push(src, dst, send, recv, kk, tt):
        same = jnp.logical_and(kk == k, tt == t)

        @pl.when(jnp.logical_not(same))
        def _():
            remote(src, dst, send, recv, kk, tt).start()

        @pl.when(same)
        def _():
            pltpu.make_async_copy(src, dst, recv).start()

    def pushed(src, dst, send, recv, kk, tt):
        same = jnp.logical_and(kk == k, tt == t)

        @pl.when(jnp.logical_not(same))
        def _():
            remote(src, dst, send, recv, kk, tt).wait_send()

    def each(count, body):
        def step(i, carry):
            body(i)
            return carry

        lax.fori_loop(0, count, step, 0)

    def arrive(buffer, sems, count):
        each(
            count,
            lambda i: pltpu.make_async_copy(buffer.at[i], buffer.at[i], sems.at[i]).wait(),
        )

    for i in range(3):
        loads[i].wait()
    scaled = (tok[...].astype(F32) * tgain[...]).astype(BF16)
    query = jnp.dot(scaled, wq[...], preferred_element_type=F32)
    if query.shape[1] % LANES:
        pad = LANES - query.shape[1] % LANES
        query = jnp.concatenate([query, jnp.zeros((batch, pad), F32)], axis=1)
    for dest in range(kv):
        group, head = dest // per_row, (dest % per_row) % lh
        first = head * head_w // LANES * LANES
        q_send[dest] = query[group * seqs : (group + 1) * seqs, first : first + chunk]
    wide = scaled.astype(F32)
    for group in range(tp):
        scaled_s[group] = wide[group * seqs : (group + 1) * seqs]
    own = scaled_s[t].astype(BF16)
    loads[3].wait()
    loads[4].wait()
    lat = jnp.dot(own, wd[...], preferred_element_type=F32)
    rope = jnp.dot(own, wr[...], preferred_element_type=F32)
    for i in range(seqs):
        lat_send[i, :, :latent] = lat[i : i + 1]
        lat_send[i, :, latent:] = jnp.zeros((1, LANES), F32)
        lat_send[i, :, latent : latent + rope_w] = rope[i : i + 1]

    pl.semaphore_wait(barrier, kv * tp - 1)

    q_args = lambda i: (q_send.at[i], q_recv.at[k], q_ss.at[i], q_rs.at[k], i, t)
    lat_args = lambda i: (
        lat_send.at[i // lat_dup],
        lat_recv.at[k],
        lat_ss.at[i],
        lat_rs.at[k],
        i,
        t,
    )
    each(kv, lambda i: push(*q_args(i)))
    each(kv, lambda i: push(*lat_args(i)))

    group = k // per_row
    head = (k % per_row) % lh
    copy_at = (k % per_row) // lh
    for i in range(5, 8):
        loads[i].wait()
    arrive(q_recv, q_rs, kv)
    query = q_recv[0]
    for i in range(1, kv):
        query = query + q_recv[i]
    query = rounded(query)
    if lh > 1:
        shift = head * head_w % LANES
        query = jnp.where(shift == 0, query, pltpu.roll(query, chunk - head_w % LANES, 1))
    spun = rotated(query[:, nope_w : nope_w + LANES], cos[group], sin[group], half)
    ql_send[:, :latent] = dot_t(query[:, :nope_w].astype(BF16), wku[head]).astype(BF16)
    ql_send[:, latent:] = spun.astype(BF16)
    ql_args = lambda i: (
        ql_send,
        ql_recv.at[t * lh + head],
        ql_ss.at[i],
        ql_rs.at[t * lh + head],
        copy_at + dup * i,
        group,
    )
    each(kv // dup, lambda i: push(*ql_args(i)))

    loads[8].wait()
    arrive(lat_recv, lat_rs, kv)
    fresh = lat_recv[0]
    for i in range(1, kv):
        fresh = fresh + lat_recv[i]
    fresh_lat = fresh[:, :latent]
    scale = lax.rsqrt(jnp.mean(fresh_lat * fresh_lat, axis=1, keepdims=True) + EPSILON)
    seq = k // lat_dup
    pick = lax.broadcasted_iota(jnp.int32, (seqs, LANES), 0) == seq
    own_cos = jnp.sum(jnp.where(pick, cos[t], 0.0), axis=0, keepdims=True)
    own_sin = jnp.sum(jnp.where(pick, sin[t], 0.0), axis=0, keepdims=True)
    row_send[:, :latent] = rounded(fresh_lat * scale * lgain[...])
    row_send[:, latent:] = rounded(rotated(fresh[:, latent:], own_cos, own_sin, half))
    row_args = lambda i: (
        row_send,
        row_recv.at[seq],
        row_ss.at[i],
        row_rs.at[seq],
        k % lat_dup + lat_dup * i,
        t,
    )
    each(kv // lat_dup, lambda i: push(*row_args(i)))

    loads[9].wait()
    loads[10].wait()
    arrive(ql_recv, ql_rs, heads)
    for i in range(heads):
        wide = ql_recv[i].astype(F32)
        for c in range(full // LANES):
            q32[c, i * seqs : (i + 1) * seqs, :] = wide[:, c * LANES : (c + 1) * LANES]
    place = k * pos + lax.broadcasted_iota(jnp.int32, (heads, pos), 1)
    lane = lax.broadcasted_iota(jnp.int32, (heads, LANES), 1)
    all_scores = []
    for b in range(seqs):
        q_b = jnp.concatenate(
            [q32[c, pl.ds(b, heads, stride=seqs), :] for c in range(full // LANES)], axis=1
        ).astype(BF16)
        all_scores.append(
            (dot_t(q_b[:, :latent], cl[b]) + dot_t(q_b[:, latent : latent + rope_w], cr[b]))
            * factor
        )
    for b in range(seqs):
        visible = place < lengths[t * seqs + b]
        scores = jnp.where(visible, all_scores[b], NEGATIVE)
        top = jnp.max(scores, axis=1, keepdims=True)
        weights = jnp.where(visible, jnp.exp(scores - top), 0.0)
        total = jnp.sum(weights, axis=1, keepdims=True)
        acc = jnp.dot(weights.astype(BF16), cl[b], preferred_element_type=F32)
        stats = jnp.zeros((heads, LANES), F32)
        for at, value in ((0, top), (3, total)):
            for i in range(3):
                piece = rounded(value)
                stats = jnp.where(lane == at + i, piece, stats)
                value = value - piece
        for c in range(latent // LANES):
            stage[c, pl.ds(b, heads, stride=seqs), :] = acc[:, c * LANES : (c + 1) * LANES]
        stage[latent // LANES, pl.ds(b, heads, stride=seqs), :] = stats
    for dest in range(kv):
        for c in range(full // LANES):
            part_send[dest, :, c * LANES : (c + 1) * LANES] = stage[
                c, dest * rows : (dest + 1) * rows, :
            ].astype(BF16)
    part_args = lambda i: (part_send.at[i], part_recv.at[k], part_ss.at[i], part_rs.at[k], i, t)
    each(kv, lambda i: push(*part_args(i)))

    head_at = k // parts
    part_at = k % parts
    arrive(row_recv, row_rs, seqs)
    new_key = jnp.concatenate([row_recv[i] for i in range(seqs)], axis=0)
    own_query = ql_recv[head_at].astype(F32)

    def part_of(values):
        result = values[:rows]
        for i in range(1, parts):
            result = jnp.where(part_at == i, values[i * rows : (i + 1) * rows], result)
        return result

    new_key = part_of(new_key)
    own_query = part_of(own_query)
    new_score = jnp.sum(own_query * new_key, axis=1, keepdims=True) * factor
    arrive(part_recv, part_rs, kv)
    tops, sums, accs = [], [], []
    best = new_score
    for i in range(kv):
        stats = part_recv[i, :, latent:].astype(F32)
        top = stats[:, 0:1] + stats[:, 1:2] + stats[:, 2:3]
        tops.append(top)
        sums.append(stats[:, 3:4] + stats[:, 4:5] + stats[:, 5:6])
        best = jnp.maximum(best, top)
    new_weight = jnp.exp(new_score - best)
    weighted = rounded(new_weight) * new_key[:, :latent]
    weight_sum = new_weight
    for i in range(kv):
        share = jnp.exp(tops[i] - best)
        weight_sum = weight_sum + share * sums[i]
        weighted = weighted + share * part_recv[i, :, :latent].astype(F32)
    hl_send[...] = (weighted / weight_sum).astype(BF16)
    slot = (head_at % lh) * (tp * parts) + t * parts + part_at
    hl_args = lambda i: (
        hl_send,
        hl_recv.at[slot],
        hl_ss.at[i],
        hl_rs.at[slot],
        i,
        head_at // lh,
    )
    each(kv, lambda i: push(*hl_args(i)))

    for i in range(11, 14):
        loads[i].wait()
    arrive(hl_recv, hl_rs, lh * tp * parts)
    outs = []
    for i in range(lh):
        base = i * tp * parts
        block = jnp.concatenate(
            [hl_recv[base + j].astype(F32) for j in range(tp * parts)], axis=0
        ).astype(BF16)
        outs.append(jnp.dot(block, wvu[i], preferred_element_type=F32).astype(BF16))
    head_out = outs[0] if lh == 1 else jnp.concatenate(outs, axis=1)
    mix_send[...] = jnp.dot(head_out, wo[...], preferred_element_type=F32).astype(BF16)
    mix_args = lambda i: (mix_send, mix_recv.at[t], mix_ss.at[i], mix_rs.at[t], k, i)
    each(tp, lambda i: push(*mix_args(i)))
    arrive(mix_recv, mix_rs, tp)
    mixed = mix_recv[0].astype(F32)
    for i in range(1, tp):
        mixed = mixed + mix_recv[i].astype(F32)

    squares = jnp.sum(mixed * mixed, axis=1, keepdims=True)
    diagonal = lax.broadcasted_iota(jnp.int32, (batch, LANES), 0) == lax.broadcasted_iota(
        jnp.int32, (batch, LANES), 1
    )
    sq_send[...] = jnp.broadcast_to(
        jnp.sum(jnp.where(diagonal, squares, 0.0), axis=0, keepdims=True), sq_send.shape
    )
    sq_args = lambda i: (sq_send, sq_recv.at[k], sq_ss.at[i], sq_rs.at[k], i, t)
    each(kv, lambda i: push(*sq_args(i)))
    arrive(sq_recv, sq_rs, kv)
    line = sq_recv[0]
    for i in range(1, kv):
        line = line + sq_recv[i]
    squares = jnp.sum(jnp.where(diagonal, line[0:1], 0.0), axis=1, keepdims=True)
    out[...] = (mixed * lax.rsqrt(squares / model_w + EPSILON) * ogain[...]).astype(out.dtype)

    each(kv, lambda i: pushed(*q_args(i)))
    each(kv, lambda i: pushed(*lat_args(i)))
    each(kv // dup, lambda i: pushed(*ql_args(i)))
    each(kv // lat_dup, lambda i: pushed(*row_args(i)))
    each(kv, lambda i: pushed(*part_args(i)))
    each(kv, lambda i: pushed(*hl_args(i)))
    each(tp, lambda i: pushed(*mix_args(i)))
    each(kv, lambda i: pushed(*sq_args(i)))


def on_device(
    kv,
    tp,
    tokens,
    token_gain,
    w_query,
    w_down_kv,
    w_rope_key,
    latent_gain,
    w_key_up,
    w_value_up,
    w_out,
    out_gain,
    cache_latent,
    cache_rope,
    lengths,
):
    batch = tokens.shape[0]
    lh, latent, nope_w = w_key_up.shape
    rope_w = w_rope_key.shape[1]
    seqs = cache_latent.shape[0]
    heads = lh * tp
    full = latent + LANES
    rows = heads * seqs // kv
    per_row = kv // tp
    parts = seqs // rows
    assert kv % tp == 0 and per_row % lh == 0 and kv % seqs == 0
    assert seqs % rows == 0 and batch == seqs * tp and batch <= LANES
    dup = per_row // lh
    lat_dup = kv // seqs
    chunk = -(-(nope_w + rope_w) // LANES) * LANES

    inverse_freq = 1.0 / 10000.0 ** (jnp.arange(0, rope_w, 2, dtype=F32) / rope_w)
    angles = lengths.astype(F32)[:, None] * inverse_freq[None, :]
    cosine, sine = jnp.cos(angles), jnp.sin(angles)
    blank = jnp.zeros((batch, LANES - rope_w), F32)
    cos = jnp.concatenate([cosine, cosine, blank], axis=1).reshape(tp, seqs, LANES)
    sin = jnp.concatenate([-sine, sine, blank], axis=1).reshape(tp, seqs, LANES)

    arrays = [
        tokens,
        token_gain[None, :],
        w_query,
        w_down_kv,
        w_rope_key,
        cos,
        sin,
        w_key_up,
        cache_latent,
        cache_rope,
        latent_gain[None, :],
        w_value_up,
        w_out,
        out_gain[None, :],
    ]
    columns = w_out.shape[1]
    dma = lambda n: pltpu.SemaphoreType.DMA((n,))
    slots = lh * tp * parts
    return pl.pallas_call(
        functools.partial(kernel, kv, tp),
        out_shape=jax.ShapeDtypeStruct((batch, columns), BF16),
        in_specs=[pl.BlockSpec(memory_space=pltpu.SMEM)]
        + [pl.BlockSpec(memory_space=pl.ANY)] * len(arrays),
        out_specs=pl.BlockSpec(memory_space=pltpu.VMEM),
        scratch_shapes=[pltpu.VMEM(a.shape, a.dtype) for a in arrays]
        + [
            pltpu.VMEM((tp, seqs, tokens.shape[1]), F32),
            pltpu.VMEM((kv, seqs, chunk), F32),
            pltpu.VMEM((kv, seqs, chunk), F32),
            pltpu.VMEM((seqs, 1, full), F32),
            pltpu.VMEM((kv, 1, full), F32),
            pltpu.VMEM((1, full), F32),
            pltpu.VMEM((seqs, 1, full), F32),
            pltpu.VMEM((seqs, full), BF16),
            pltpu.VMEM((heads, seqs, full), BF16),
            pltpu.VMEM((full // LANES, heads * seqs, LANES), F32),
            pltpu.VMEM((full // LANES, heads * seqs, LANES), F32),
            pltpu.VMEM((kv, rows, full), BF16),
            pltpu.VMEM((kv, rows, full), BF16),
            pltpu.VMEM((rows, latent), BF16),
            pltpu.VMEM((slots, rows, latent), BF16),
            pltpu.VMEM((batch, columns), BF16),
            pltpu.VMEM((tp, batch, columns), BF16),
            pltpu.VMEM((8, LANES), F32),
            pltpu.VMEM((kv, 8, LANES), F32),
            dma(len(arrays)),
            dma(kv),
            dma(kv),
            dma(kv),
            dma(kv),
            dma(kv // lat_dup),
            dma(seqs),
            dma(kv // dup),
            dma(heads),
            dma(kv),
            dma(kv),
            dma(kv),
            dma(slots),
            dma(tp),
            dma(tp),
            dma(kv),
            dma(kv),
        ],
        compiler_params=pltpu.CompilerParams(
            collective_id=0, has_side_effects=True, vmem_limit_bytes=56 * 1024 * 1024
        ),
        name="decode",
    )(lengths, *arrays)


def solution(mesh):
    placed = (
        P(None, "kv"),
        P("kv"),
        P("kv", "tp"),
        P("kv", None),
        P("kv", None),
        P(),
        P("tp", None, None),
        P("tp", None, None),
        P("tp", "kv"),
        P("kv"),
        P("tp", "kv", None),
        P("tp", "kv", None),
        P(),
    )
    return jax.shard_map(
        functools.partial(on_device, mesh.shape["kv"], mesh.shape["tp"]),
        mesh=mesh,
        in_specs=placed,
        out_specs=P(None, "kv"),
        check_vma=False,
    )
```

```python
import functools

import jax
import jax.numpy as jnp
from jax import lax
from jax.experimental import pallas as pl
from jax.experimental.pallas import tpu as pltpu
from jax.sharding import PartitionSpec as P

EPSILON = 1e-06
NEGATIVE = -1e30
LANES = 128
MESH = pl.DeviceIdType.MESH
F32 = jnp.float32
BF16 = jnp.bfloat16


def rounded(values):
    return values.astype(BF16).astype(F32)


def rotated(values, cosine, signed_sine, half):
    lane = lax.broadcasted_iota(jnp.int32, values.shape, 1)
    swapped = jnp.where(
        lane < half, pltpu.roll(values, LANES - half, 1), pltpu.roll(values, half, 1)
    )
    return values * cosine + swapped * signed_sine


def dot_t(a, b):
    return lax.dot_general(a, b, (((1,), (1,)), ((), ())), preferred_element_type=F32)


def kernel(
    kv,
    tp,
    lengths,
    tok_h,
    tgain_h,
    wq_h,
    wd_h,
    wr_h,
    cos_h,
    sin_h,
    wku_h,
    cl_h,
    cr_h,
    lgain_h,
    wvu_h,
    wo_h,
    ogain_h,
    out,
    tok,
    tgain,
    wq,
    wd,
    wr,
    cos,
    sin,
    wku,
    cl,
    cr,
    lgain,
    wvu,
    wo,
    ogain,
    scaled_s,
    q_send,
    q_recv,
    lat_send,
    lat_recv,
    row_send,
    row_recv,
    ql_send,
    ql_recv,
    q32,
    stage,
    part_send,
    part_recv,
    hl_send,
    hl_recv,
    mix_send,
    mix_recv,
    sq_send,
    sq_recv,
    in_sem,
    q_ss,
    q_rs,
    lat_ss,
    lat_rs,
    row_ss,
    row_rs,
    ql_ss,
    ql_rs,
    part_ss,
    part_rs,
    hl_ss,
    hl_rs,
    mix_ss,
    mix_rs,
    sq_ss,
    sq_rs,
):
    k = lax.axis_index("kv")
    t = lax.axis_index("tp")
    batch, width = tok.shape
    lh, latent, nope_w = wku.shape
    rope_w = wr.shape[0]
    head_w = nope_w + rope_w
    half = rope_w // 2
    factor = head_w ** (-0.5)
    seqs, pos = cl.shape[0], cl.shape[1]
    heads = lh * tp
    full = latent + LANES
    per_row = kv // tp
    dup = per_row // lh
    lat_dup = kv // seqs
    rows = heads * seqs // kv
    parts = seqs // rows
    model_w = width * kv
    chunk = q_send.shape[2]

    loads = [
        pltpu.make_async_copy(a, b, in_sem.at[i])
        for i, (a, b) in enumerate(
            [
                (tok_h, tok),
                (tgain_h, tgain),
                (wq_h, wq),
                (wd_h, wd),
                (wr_h, wr),
                (cos_h, cos),
                (sin_h, sin),
                (wku_h, wku),
                (lgain_h, lgain),
                (cl_h, cl),
                (cr_h, cr),
                (wvu_h, wvu),
                (wo_h, wo),
                (ogain_h, ogain),
            ]
        )
    ]
    for load in loads:
        load.start()

    barrier = pltpu.get_barrier_semaphore()
    me = k * tp + t

    def greet(i, carry):
        @pl.when(i != me)
        def _():
            pl.semaphore_signal(
                barrier, inc=1, device_id=(i // tp, i % tp), device_id_type=MESH
            )

        return carry

    lax.fori_loop(0, kv * tp, greet, 0)

    def remote(src, dst, send, recv, kk, tt):
        return pltpu.make_async_remote_copy(
            src_ref=src,
            dst_ref=dst,
            send_sem=send,
            recv_sem=recv,
            device_id=(kk, tt),
            device_id_type=MESH,
        )

    def push(src, dst, send, recv, kk, tt):
        same = jnp.logical_and(kk == k, tt == t)

        @pl.when(jnp.logical_not(same))
        def _():
            remote(src, dst, send, recv, kk, tt).start()

        @pl.when(same)
        def _():
            pltpu.make_async_copy(src, dst, recv).start()

    def pushed(src, dst, send, recv, kk, tt):
        same = jnp.logical_and(kk == k, tt == t)

        @pl.when(jnp.logical_not(same))
        def _():
            remote(src, dst, send, recv, kk, tt).wait_send()

    def each(count, body):
        def step(i, carry):
            body(i)
            return carry

        lax.fori_loop(0, count, step, 0)

    def arrive(buffer, sems, count):
        each(
            count,
            lambda i: pltpu.make_async_copy(buffer.at[i], buffer.at[i], sems.at[i]).wait(),
        )

    for i in range(3):
        loads[i].wait()
    scaled = (tok[...].astype(F32) * tgain[...]).astype(BF16)
    query = jnp.dot(scaled, wq[...], preferred_element_type=F32)
    if query.shape[1] % LANES:
        pad = LANES - query.shape[1] % LANES
        query = jnp.concatenate([query, jnp.zeros((batch, pad), F32)], axis=1)
    for dest in range(kv):
        group, head = dest // per_row, (dest % per_row) % lh
        first = head * head_w // LANES * LANES
        q_send[dest] = query[group * seqs : (group + 1) * seqs, first : first + chunk]
    wide = scaled.astype(F32)
    for group in range(tp):
        scaled_s[group] = wide[group * seqs : (group + 1) * seqs]
    own = scaled_s[t].astype(BF16)
    loads[3].wait()
    loads[4].wait()
    lat = jnp.dot(own, wd[...], preferred_element_type=F32)
    rope = dot_t(own, wr[...])
    for i in range(seqs):
        lat_send[i, :, :latent] = lat[i : i + 1]
        lat_send[i, :, latent:] = jnp.zeros((1, LANES), F32)
        lat_send[i, :, latent : latent + rope_w] = rope[i : i + 1]

    pl.semaphore_wait(barrier, kv * tp - 1)

    q_args = lambda i: (q_send.at[i], q_recv.at[k], q_ss.at[i], q_rs.at[k], i, t)
    lat_args = lambda i: (
        lat_send.at[i // lat_dup],
        lat_recv.at[k],
        lat_ss.at[i],
        lat_rs.at[k],
        i,
        t,
    )
    each(kv, lambda i: push(*q_args(i)))
    each(kv, lambda i: push(*lat_args(i)))

    group = k // per_row
    head = (k % per_row) % lh
    copy_at = (k % per_row) // lh
    for i in range(5, 8):
        loads[i].wait()
    arrive(q_recv, q_rs, kv)
    query = q_recv[0]
    for i in range(1, kv):
        query = query + q_recv[i]
    query = rounded(query)
    if lh > 1:
        shift = head * head_w % LANES
        query = jnp.where(shift == 0, query, pltpu.roll(query, chunk - head_w % LANES, 1))
    spun = rotated(query[:, nope_w : nope_w + LANES], cos[group], sin[group], half)
    ql_send[:, :latent] = dot_t(query[:, :nope_w].astype(BF16), wku[head]).astype(BF16)
    ql_send[:, latent:] = spun.astype(BF16)
    ql_args = lambda i: (
        ql_send,
        ql_recv.at[t * lh + head],
        ql_ss.at[i],
        ql_rs.at[t * lh + head],
        copy_at + dup * i,
        group,
    )
    each(kv // dup, lambda i: push(*ql_args(i)))

    loads[8].wait()
    arrive(lat_recv, lat_rs, kv)
    fresh = lat_recv[0]
    for i in range(1, kv):
        fresh = fresh + lat_recv[i]
    fresh_lat = fresh[:, :latent]
    scale = lax.rsqrt(jnp.mean(fresh_lat * fresh_lat, axis=1, keepdims=True) + EPSILON)
    seq = k // lat_dup
    pick = lax.broadcasted_iota(jnp.int32, (seqs, LANES), 0) == seq
    own_cos = jnp.sum(jnp.where(pick, cos[t], 0.0), axis=0, keepdims=True)
    own_sin = jnp.sum(jnp.where(pick, sin[t], 0.0), axis=0, keepdims=True)
    row_send[:, :latent] = rounded(fresh_lat * scale * lgain[...])
    row_send[:, latent:] = rounded(rotated(fresh[:, latent:], own_cos, own_sin, half))
    row_args = lambda i: (
        row_send,
        row_recv.at[seq],
        row_ss.at[i],
        row_rs.at[seq],
        k % lat_dup + lat_dup * i,
        t,
    )
    each(kv // lat_dup, lambda i: push(*row_args(i)))

    loads[9].wait()
    loads[10].wait()
    arrive(ql_recv, ql_rs, heads)
    for i in range(heads):
        wide = ql_recv[i].astype(F32)
        for c in range(full // LANES):
            q32[c, i * seqs : (i + 1) * seqs, :] = wide[:, c * LANES : (c + 1) * LANES]
    place = k * pos + lax.broadcasted_iota(jnp.int32, (heads, pos), 1)
    lane = lax.broadcasted_iota(jnp.int32, (heads, LANES), 1)
    all_scores = []
    for b in range(seqs):
        q_b = jnp.concatenate(
            [q32[c, pl.ds(b, heads, stride=seqs), :] for c in range(full // LANES)], axis=1
        ).astype(BF16)
        all_scores.append(
            (
                dot_t(q_b[:, :latent], cl[b])
                + jnp.dot(
                    q_b[:, latent : latent + rope_w], cr[b], preferred_element_type=F32
                )
            )
            * factor
        )
    for b in range(seqs):
        visible = place < lengths[t * seqs + b]
        scores = jnp.where(visible, all_scores[b], NEGATIVE)
        top = jnp.max(scores, axis=1, keepdims=True)
        weights = jnp.where(visible, jnp.exp(scores - top), 0.0)
        total = jnp.sum(weights, axis=1, keepdims=True)
        acc = jnp.dot(weights.astype(BF16), cl[b], preferred_element_type=F32)
        stats = jnp.zeros((heads, LANES), F32)
        for at, value in ((0, top), (3, total)):
            for i in range(3):
                piece = rounded(value)
                stats = jnp.where(lane == at + i, piece, stats)
                value = value - piece
        for c in range(latent // LANES):
            stage[c, pl.ds(b, heads, stride=seqs), :] = acc[:, c * LANES : (c + 1) * LANES]
        stage[latent // LANES, pl.ds(b, heads, stride=seqs), :] = stats
    for dest in range(kv):
        for c in range(full // LANES):
            part_send[dest, :, c * LANES : (c + 1) * LANES] = stage[
                c, dest * rows : (dest + 1) * rows, :
            ].astype(BF16)
    part_args = lambda i: (part_send.at[i], part_recv.at[k], part_ss.at[i], part_rs.at[k], i, t)
    each(kv, lambda i: push(*part_args(i)))

    head_at = k // parts
    part_at = k % parts
    arrive(row_recv, row_rs, seqs)
    new_key = jnp.concatenate([row_recv[i] for i in range(seqs)], axis=0)
    own_query = ql_recv[head_at].astype(F32)

    def part_of(values):
        result = values[:rows]
        for i in range(1, parts):
            result = jnp.where(part_at == i, values[i * rows : (i + 1) * rows], result)
        return result

    new_key = part_of(new_key)
    own_query = part_of(own_query)
    new_score = jnp.sum(own_query * new_key, axis=1, keepdims=True) * factor
    arrive(part_recv, part_rs, kv)
    tops, sums, accs = [], [], []
    best = new_score
    for i in range(kv):
        stats = part_recv[i, :, latent:].astype(F32)
        top = stats[:, 0:1] + stats[:, 1:2] + stats[:, 2:3]
        tops.append(top)
        sums.append(stats[:, 3:4] + stats[:, 4:5] + stats[:, 5:6])
        best = jnp.maximum(best, top)
    new_weight = jnp.exp(new_score - best)
    weighted = rounded(new_weight) * new_key[:, :latent]
    weight_sum = new_weight
    for i in range(kv):
        share = jnp.exp(tops[i] - best)
        weight_sum = weight_sum + share * sums[i]
        weighted = weighted + share * part_recv[i, :, :latent].astype(F32)
    hl_send[...] = (weighted / weight_sum).astype(BF16)
    slot = (head_at % lh) * (tp * parts) + t * parts + part_at
    hl_args = lambda i: (
        hl_send,
        hl_recv.at[slot],
        hl_ss.at[i],
        hl_rs.at[slot],
        i,
        head_at // lh,
    )
    each(kv, lambda i: push(*hl_args(i)))

    for i in range(11, 14):
        loads[i].wait()
    arrive(hl_recv, hl_rs, lh * tp * parts)
    outs = []
    for i in range(lh):
        base = i * tp * parts
        block = jnp.concatenate(
            [hl_recv[base + j].astype(F32) for j in range(tp * parts)], axis=0
        ).astype(BF16)
        outs.append(jnp.dot(block, wvu[i], preferred_element_type=F32).astype(BF16))
    head_out = outs[0] if lh == 1 else jnp.concatenate(outs, axis=1)
    mix_send[...] = jnp.dot(head_out, wo[...], preferred_element_type=F32).astype(BF16)
    mix_args = lambda i: (mix_send, mix_recv.at[t], mix_ss.at[i], mix_rs.at[t], k, i)
    each(tp, lambda i: push(*mix_args(i)))
    arrive(mix_recv, mix_rs, tp)
    mixed = mix_recv[0].astype(F32)
    for i in range(1, tp):
        mixed = mixed + mix_recv[i].astype(F32)

    squares = jnp.sum(mixed * mixed, axis=1, keepdims=True)
    diagonal = lax.broadcasted_iota(jnp.int32, (batch, LANES), 0) == lax.broadcasted_iota(
        jnp.int32, (batch, LANES), 1
    )
    sq_send[...] = jnp.broadcast_to(
        jnp.sum(jnp.where(diagonal, squares, 0.0), axis=0, keepdims=True), sq_send.shape
    )
    sq_args = lambda i: (sq_send, sq_recv.at[k], sq_ss.at[i], sq_rs.at[k], i, t)
    each(kv, lambda i: push(*sq_args(i)))
    arrive(sq_recv, sq_rs, kv)
    line = sq_recv[0]
    for i in range(1, kv):
        line = line + sq_recv[i]
    squares = jnp.sum(jnp.where(diagonal, line[0:1], 0.0), axis=1, keepdims=True)
    out[...] = (mixed * lax.rsqrt(squares / model_w + EPSILON) * ogain[...]).astype(out.dtype)

    each(kv, lambda i: pushed(*q_args(i)))
    each(kv, lambda i: pushed(*lat_args(i)))
    each(kv // dup, lambda i: pushed(*ql_args(i)))
    each(kv // lat_dup, lambda i: pushed(*row_args(i)))
    each(kv, lambda i: pushed(*part_args(i)))
    each(kv, lambda i: pushed(*hl_args(i)))
    each(tp, lambda i: pushed(*mix_args(i)))
    each(kv, lambda i: pushed(*sq_args(i)))


def on_device(
    kv,
    tp,
    tokens,
    token_gain,
    w_query,
    w_down_kv,
    w_rope_key,
    latent_gain,
    w_key_up,
    w_value_up,
    w_out,
    out_gain,
    cache_latent,
    cache_rope,
    lengths,
):
    batch = tokens.shape[0]
    lh, latent, nope_w = w_key_up.shape
    rope_w = w_rope_key.shape[1]
    seqs = cache_latent.shape[0]
    heads = lh * tp
    full = latent + LANES
    rows = heads * seqs // kv
    per_row = kv // tp
    parts = seqs // rows
    assert kv % tp == 0 and per_row % lh == 0 and kv % seqs == 0
    assert seqs % rows == 0 and batch == seqs * tp and batch <= LANES
    dup = per_row // lh
    lat_dup = kv // seqs
    chunk = -(-(nope_w + rope_w) // LANES) * LANES

    inverse_freq = 1.0 / 10000.0 ** (jnp.arange(0, rope_w, 2, dtype=F32) / rope_w)
    angles = lengths.astype(F32)[:, None] * inverse_freq[None, :]
    cosine, sine = jnp.cos(angles), jnp.sin(angles)
    blank = jnp.zeros((batch, LANES - rope_w), F32)
    cos = jnp.concatenate([cosine, cosine, blank], axis=1).reshape(tp, seqs, LANES)
    sin = jnp.concatenate([-sine, sine, blank], axis=1).reshape(tp, seqs, LANES)

    arrays = [
        tokens,
        token_gain[None, :],
        w_query,
        w_down_kv,
        w_rope_key.T,
        cos,
        sin,
        w_key_up,
        cache_latent,
        jnp.swapaxes(cache_rope, 1, 2),
        latent_gain[None, :],
        w_value_up,
        w_out,
        out_gain[None, :],
    ]
    columns = w_out.shape[1]
    dma = lambda n: pltpu.SemaphoreType.DMA((n,))
    slots = lh * tp * parts
    return pl.pallas_call(
        functools.partial(kernel, kv, tp),
        out_shape=jax.ShapeDtypeStruct((batch, columns), BF16),
        in_specs=[pl.BlockSpec(memory_space=pltpu.SMEM)]
        + [pl.BlockSpec(memory_space=pl.ANY)] * len(arrays),
        out_specs=pl.BlockSpec(memory_space=pltpu.VMEM),
        scratch_shapes=[pltpu.VMEM(a.shape, a.dtype) for a in arrays]
        + [
            pltpu.VMEM((tp, seqs, tokens.shape[1]), F32),
            pltpu.VMEM((kv, seqs, chunk), F32),
            pltpu.VMEM((kv, seqs, chunk), F32),
            pltpu.VMEM((seqs, 1, full), F32),
            pltpu.VMEM((kv, 1, full), F32),
            pltpu.VMEM((1, full), F32),
            pltpu.VMEM((seqs, 1, full), F32),
            pltpu.VMEM((seqs, full), BF16),
            pltpu.VMEM((heads, seqs, full), BF16),
            pltpu.VMEM((full // LANES, heads * seqs, LANES), F32),
            pltpu.VMEM((full // LANES, heads * seqs, LANES), F32),
            pltpu.VMEM((kv, rows, full), BF16),
            pltpu.VMEM((kv, rows, full), BF16),
            pltpu.VMEM((rows, latent), BF16),
            pltpu.VMEM((slots, rows, latent), BF16),
            pltpu.VMEM((batch, columns), BF16),
            pltpu.VMEM((tp, batch, columns), BF16),
            pltpu.VMEM((8, LANES), F32),
            pltpu.VMEM((kv, 8, LANES), F32),
            dma(len(arrays)),
            dma(kv),
            dma(kv),
            dma(kv),
            dma(kv),
            dma(kv // lat_dup),
            dma(seqs),
            dma(kv // dup),
            dma(heads),
            dma(kv),
            dma(kv),
            dma(kv),
            dma(slots),
            dma(tp),
            dma(tp),
            dma(kv),
            dma(kv),
        ],
        compiler_params=pltpu.CompilerParams(
            collective_id=0, has_side_effects=True, vmem_limit_bytes=56 * 1024 * 1024
        ),
        name="decode",
    )(lengths, *arrays)


def solution(mesh):
    placed = (
        P(None, "kv"),
        P("kv"),
        P("kv", "tp"),
        P("kv", None),
        P("kv", None),
        P(),
        P("tp", None, None),
        P("tp", None, None),
        P("tp", "kv"),
        P("kv"),
        P("tp", "kv", None),
        P("tp", "kv", None),
        P(),
    )
    return jax.shard_map(
        functools.partial(on_device, mesh.shape["kv"], mesh.shape["tp"]),
        mesh=mesh,
        in_specs=placed,
        out_specs=P(None, "kv"),
        check_vma=False,
    )
```
